32 devices in a mesh: fs: 16 (over z, y, x), tp: 2 (over core).
Axes of the slice: x: 2, y: 2, z: 4, core: 2. Of those that a mesh axis runs over, the one named last changes fastest.
Arguments:
- tokens: bfloat16 [6144, 2048], P('fs', 'tp'), may hold values from -24 to 24, as said below
- mixer_gain: float32 [2048], replicated, may hold values from 0.1 to 1.9
- w_content: float32 [2048, 1024], P('fs', 'tp'), may hold values from -0.125 to 0.125
- w_spatial: float32 [2048, 1024], P('fs', 'tp'), may hold values from -0.125 to 0.125
- content_scale: float32 [1024], P('tp'), may hold values from 0.5 to 2
- spatial_scale: float32 [1024], P('tp'), may hold values from 0.2 to 3.5, as said below
- spatial_gain: float32 [1024], P('tp'), may hold values from 0.1 to 1.9
- block_mixing: bfloat16 [8, 128, 128], P('tp'), may hold values from -0.5 to 0.5
- block_bias: float32 [8, 128], P('tp'), may hold values from -6 to 6
- w_project: float32 [1024, 2048], P('tp', 'fs'), may hold values from -0.1875 to 0.1875
- project_scale: float32 [2048], P('fs'), may hold values from 0.5 to 2
- channel_gain: float32 [2048], replicated, may hold values from 0.1 to 1.9
- w_up: float32 [2048, 8192], P('fs', 'tp'), may hold values from -0.125 to 0.125
- up_scale: float32 [8192], P('tp'), may hold values from 0.5 to 2
- w_down: float32 [8192, 2048], P('tp', 'fs'), may hold values from -0.0625 to 0.0625
- down_scale: float32 [2048], P('fs'), may hold values from 0.5 to 2
Outputs:
- layer_out: bfloat16 [6144, 2048], P('fs', 'tp')
The draws below stay inside these ranges and needn't reach their ends.
Inputs may be any that keep to these rules, and one draw needn't show every extreme that they name: `tokens`: activations whose features and rows have differing scales. `spatial_scale`: positive column scales.
All inputs are finite; a program needn't handle non-finite values.
Results may differ from the reference program's by a relative error of at most 0.019.
Values may be sent and summed in bfloat16 or wider, within the bound.
A program may use at most 128 MiB of HBM per device.

```python
import math
import jax
import jax.numpy as jnp
from jax import lax

D = 2048
GROUPS = 8
GCH = 128
W_SGU = 1024
FF = 8192
BLOCK = 128
TOK_DEV = 384
TOKENS = 6144
N_FS = 16
N_TP = 2


def draw_tokens(key, part):
    first_key = jax.random.fold_in(key, 11)
    second_key = jax.random.fold_in(key, 12)
    third_key = jax.random.fold_in(key, 13)
    column_scales = jnp.exp(jax.random.uniform(second_key, (D,), jnp.float32, math.log(0.3), math.log(3.0)))
    base_values = jax.random.truncated_normal(first_key, -4.0, 4.0, (TOKENS, D), jnp.float32)
    row_scales = jnp.exp(jax.random.uniform(third_key, (TOKENS, 1), jnp.float32, math.log(0.5), math.log(2.0)))
    return (base_values * column_scales[None, :] * row_scales).astype(jnp.bfloat16)


def draw_spatial_scale(key, part):
    jitter_key = jax.random.fold_in(key, 21)
    position = jnp.arange(W_SGU).astype(jnp.float32) / (W_SGU - 1)
    jitter = jnp.exp(jax.random.uniform(jitter_key, (W_SGU,), jnp.float32, -0.35, 0.35))
    base_scale = jnp.exp(math.log(0.5) + (math.log(1.6) - math.log(0.5)) * position)
    return (base_scale * jitter).astype(jnp.float32)


def shard_levels(own_key, dims, shards, smallest, largest):
    factor_of = 1.0
    for dim, blocks in shards:
        heights = jax.random.uniform(jax.random.fold_in(jax.random.fold_in(own_key, 6), dim), (blocks,), jnp.float32, smallest / len(shards), largest / len(shards))
        factor_of = factor_of * jnp.repeat(jnp.exp(heights), dims[dim] // blocks).reshape((-1,) + (1,) * (len(dims) - 1 - dim))
    return factor_of


def scatter_about(stream_key, dims, scale, reach, split=(), kind=jnp.bfloat16):
    values = scale * jax.random.normal(stream_key, dims, jnp.float32)
    if split:
        values = values * shard_levels(stream_key, dims, split, -0.22, 0.18)
    return jnp.clip(values, -reach, reach).astype(kind)


def setup_inputs(seed: int = 0) -> dict:
    seeds = jax.random.split(jax.random.key(seed), 17)
    return {
        "tokens": draw_tokens(jax.random.fold_in(seeds[16], 71), 0),
        "mixer_gain": jnp.clip(1.0 + 0.18 * jax.random.normal(seeds[1], (D,), jnp.float32), 0.1, 1.9),
        "w_content": scatter_about(seeds[2], (D, W_SGU), D ** -0.5, 0.125, ((0, 16), (1, 2)), jnp.float32),
        "w_spatial": scatter_about(seeds[3], (D, W_SGU), D ** -0.5, 0.125, ((0, 16), (1, 2)), jnp.float32),
        "content_scale": jnp.clip(jnp.exp(math.log(2.0) - 1.3862944 * jax.random.uniform(seeds[4], (W_SGU,), jnp.float32) ** shard_levels(seeds[4], (W_SGU,), ((0, 2),), -0.2, 0.2)), 0.5, 2.0),
        "spatial_scale": draw_spatial_scale(jax.random.fold_in(seeds[16], 71), 0),
        "spatial_gain": jnp.clip(1.0 + 0.18 * jax.random.normal(seeds[6], (W_SGU,), jnp.float32), 0.1, 1.9),
        "block_mixing": scatter_about(seeds[7], (GROUPS, BLOCK, BLOCK), BLOCK ** -0.5, 0.5, ((0, 2),)),
        "block_bias": scatter_about(seeds[8], (GROUPS, BLOCK), 1.0, 6.0, ((0, 2),), jnp.float32),
        "w_project": scatter_about(seeds[9], (W_SGU, D), W_SGU ** -0.5, 0.1875, ((0, 2), (1, 16)), jnp.float32),
        "project_scale": jnp.clip(jnp.exp(math.log(2.0) - 1.3862944 * jax.random.uniform(seeds[10], (D,), jnp.float32) ** shard_levels(seeds[10], (D,), ((0, 16),), -0.2, 0.2)), 0.5, 2.0),
        "channel_gain": jnp.clip(1.0 + 0.18 * jax.random.normal(seeds[11], (D,), jnp.float32), 0.1, 1.9),
        "w_up": scatter_about(seeds[12], (D, FF), D ** -0.5, 0.125, ((0, 16), (1, 2)), jnp.float32),
        "up_scale": jnp.clip(jnp.exp(math.log(2.0) - 1.3862944 * jax.random.uniform(seeds[13], (FF,), jnp.float32) ** shard_levels(seeds[13], (FF,), ((0, 2),), -0.2, 0.2)), 0.5, 2.0),
        "w_down": scatter_about(seeds[14], (FF, D), FF ** -0.5, 0.0625, ((0, 2), (1, 16)), jnp.float32),
        "down_scale": jnp.clip(jnp.exp(math.log(2.0) - 1.3862944 * jax.random.uniform(seeds[15], (D,), jnp.float32) ** shard_levels(seeds[15], (D,), ((0, 16),), -0.2, 0.2)), 0.5, 2.0),
    }


EPSILON = 1e-06

def normalize_rows(token_rows, gain_vector):
    values = token_rows.astype(jnp.float32)
    scaled = values * lax.rsqrt(lax.optimization_barrier(jnp.mean(values * values, axis=-1, keepdims=True)) + EPSILON)
    return (scaled * gain_vector).astype(jnp.bfloat16)

def split_sum(left, right, column_scale, shard_count):
    shard_width = left.shape[1] // shard_count
    running = jnp.zeros((left.shape[0], right.shape[1]), jnp.float32)
    for shard_index in range(shard_count):
        low = shard_index * shard_width
        partial_value = jnp.dot(left[:, low:low + shard_width], right[low:low + shard_width, :], preferred_element_type=jnp.float32) * column_scale
        rounded = lax.optimization_barrier(partial_value.astype(jnp.bfloat16))
        running = running + rounded.astype(jnp.float32)
    return running

def reference(tokens, mixer_gain, w_content, w_spatial, content_scale, spatial_scale, spatial_gain, block_mixing, block_bias, w_project, project_scale, channel_gain, w_up, up_scale, w_down, down_scale):
    content_weight = w_content.astype(jnp.bfloat16)
    spatial_weight = w_spatial.astype(jnp.bfloat16)
    project_weight = w_project.astype(jnp.bfloat16)
    up_weight = w_up.astype(jnp.bfloat16)
    down_weight = w_down.astype(jnp.bfloat16)
    causal_mask = jnp.tril(jnp.ones((BLOCK, BLOCK), dtype=bool))
    mixing_weights = jnp.where(causal_mask[None, :, :], block_mixing.astype(jnp.float32), jnp.float32(0.0))

    def one_sequence(token_rows):
        normed = normalize_rows(token_rows, mixer_gain)
        content = jax.nn.gelu(jnp.dot(normed, content_weight, preferred_element_type=jnp.float32) * content_scale)
        spatial = jax.nn.gelu(jnp.dot(normed, spatial_weight, preferred_element_type=jnp.float32) * spatial_scale)
        spatial_norm = (spatial * lax.rsqrt(lax.optimization_barrier(jnp.mean(spatial * spatial, axis=-1, keepdims=True)) + EPSILON) * spatial_gain).astype(jnp.bfloat16)
        grouped = spatial_norm.astype(jnp.float32).reshape(TOK_DEV // BLOCK, BLOCK, GROUPS, GCH)
        mixed_block = jnp.einsum('gts,nsgc->ntgc', mixing_weights, grouped) + block_bias.T[None, :, :, None]
        gated = (content * mixed_block.reshape(TOK_DEV, W_SGU)).astype(jnp.bfloat16)
        mixer_sum = split_sum(gated, project_weight, project_scale, N_TP)
        middle = (token_rows.astype(jnp.float32) + mixer_sum).astype(jnp.bfloat16)
        channel_normed = normalize_rows(middle, channel_gain)
        up_linear = jnp.dot(channel_normed, up_weight, preferred_element_type=jnp.float32) * up_scale
        hidden = jnp.square(jax.nn.relu(up_linear)).astype(jnp.bfloat16)
        channel_sum = split_sum(hidden, down_weight, down_scale, N_TP)
        return (middle.astype(jnp.float32) + channel_sum).astype(jnp.bfloat16)
    layer_out = lax.map(one_sequence, tokens.reshape(N_FS, TOK_DEV, D))
    return layer_out.reshape(TOKENS, D)
```

```python
import functools

import jax
import jax.numpy as jnp
from jax import lax
from jax.experimental import pallas as pl
from jax.experimental.pallas import tpu as pltpu
from jax.sharding import PartitionSpec as P

EPSILON = 1e-06


def normalize_rows(token_rows, gain_vector):
    values = token_rows.astype(jnp.float32)
    scaled = values * lax.rsqrt(jnp.mean(values * values, axis=-1, keepdims=True) + EPSILON)
    return (scaled * gain_vector).astype(jnp.bfloat16)


def shards(
    tokens,
    mixer_gain,
    w_content,
    w_spatial,
    content_scale,
    spatial_scale,
    spatial_gain,
    block_mixing,
    block_bias,
    w_project,
    project_scale,
    channel_gain,
    w_up,
    up_scale,
    w_down,
    down_scale,
):
    content_weight = w_content.astype(jnp.bfloat16)
    spatial_weight = w_spatial.astype(jnp.bfloat16)
    project_weight = w_project.astype(jnp.bfloat16)
    up_weight = w_up.astype(jnp.bfloat16)
    down_weight = w_down.astype(jnp.bfloat16)
    project_full, down_full = (
        lax.all_gather(project_scale, "fs", axis=0, tiled=True),
        lax.all_gather(down_scale, "fs", axis=0, tiled=True),
    )
    gathered_rows = lax.all_gather(tokens, "tp", axis=1, tiled=True)
    normed = normalize_rows(gathered_rows, mixer_gain)
    row_count = gathered_rows.shape[0]
    content_full, spatial_full, project_cols = (
        lax.all_gather(content_weight, "fs", axis=0, tiled=True),
        lax.all_gather(spatial_weight, "fs", axis=0, tiled=True),
        lax.all_gather(project_weight, "fs", axis=1, tiled=True),
    )
    content_linear = jnp.dot(normed, content_full, preferred_element_type=jnp.float32)
    spatial_linear = jnp.dot(normed, spatial_full, preferred_element_type=jnp.float32)
    content = jax.nn.gelu(content_linear * content_scale)
    spatial = jax.nn.gelu(spatial_linear * spatial_scale)
    square_sums = lax.psum(jnp.sum(spatial * spatial, axis=1), "tp")
    total_width = spatial.shape[1] * lax.axis_size("tp")
    spatial_norm = (
        spatial * lax.rsqrt(square_sums / total_width + EPSILON)[:, None] * spatial_gain
    ).astype(jnp.bfloat16)
    groups_here = block_mixing.shape[0]
    block_size = block_mixing.shape[1]
    group_width = spatial_norm.shape[1] // groups_here
    causal_mask = jnp.tril(jnp.ones((block_size, block_size), dtype=bool))
    mixing_weights = jnp.where(causal_mask[None, :, :], block_mixing, jnp.zeros_like(block_mixing))
    grouped = spatial_norm.reshape(row_count // block_size, block_size, groups_here, group_width)
    mixed_block = (
        jnp.einsum("gts,nsgc->ntgc", mixing_weights, grouped, preferred_element_type=jnp.float32)
        + block_bias.T[None, :, :, None]
    )
    gated = (content * mixed_block.reshape(row_count, spatial_norm.shape[1])).astype(jnp.bfloat16)
    mixer_terms = jnp.dot(gated, project_cols, preferred_element_type=jnp.float32) * project_full
    mixer_sum = lax.psum_scatter(
        mixer_terms.astype(jnp.bfloat16), "tp", scatter_dimension=1, tiled=True
    ).astype(jnp.float32)
    middle = (tokens.astype(jnp.float32) + mixer_sum).astype(jnp.bfloat16)
    middle_rows = lax.all_gather(middle, "tp", axis=1, tiled=True)
    channel_normed = normalize_rows(middle_rows, channel_gain)
    up_full, down_cols = (
        lax.all_gather(up_weight, "fs", axis=0, tiled=True),
        lax.all_gather(down_weight, "fs", axis=1, tiled=True),
    )
    up_linear = jnp.dot(channel_normed, up_full, preferred_element_type=jnp.float32)
    hidden = jnp.square(jax.nn.relu(up_linear * up_scale)).astype(jnp.bfloat16)
    channel_terms = jnp.dot(hidden, down_cols, preferred_element_type=jnp.float32) * down_full
    channel_sum = lax.psum_scatter(
        channel_terms.astype(jnp.bfloat16), "tp", scatter_dimension=1, tiled=True
    ).astype(jnp.float32)
    return (middle.astype(jnp.float32) + channel_sum).astype(jnp.bfloat16)


PLANE = 4
MESH = pl.DeviceIdType.MESH


def layer_kernel(
    sizes,
    tokens_ref,
    mixer_gain_ref,
    content_ref,
    spatial_ref,
    content_scale_ref,
    spatial_scale_ref,
    spatial_gain_ref,
    mixing_ref,
    bias_ref,
    project_ref,
    project_scale_ref,
    channel_gain_ref,
    up_ref,
    up_scale_ref,
    down_ref,
    down_scale_ref,
    out_ref,
    token_rows,
    normed,
    gate_weights,
    project_full,
    up_own,
    down_own,
    up_full,
    down_full,
    content_buf,
    spatial_buf,
    gated,
    sums,
    sums_in,
    part,
    part_in,
    middle,
    rows_all,
    hidden,
    terms,
    terms_in,
    results_in,
    pair_send,
    pair_recv,
    swap_send,
    swap_recv,
    line_send,
    line_recv,
    gate_line_send,
    gate_line_recv,
    gate_send,
    gate_recv,
    row_send,
    row_recv,
    fwd_send,
    fwd_recv,
    term_send,
    term_recv,
    result_send,
    result_recv,
):
    lines = sizes["lines"]
    rows, half = tokens_ref.shape
    width = token_rows.shape[1]
    depth = content_ref.shape[0]
    channels = content_ref.shape[1]
    units = up_full.shape[1]
    band = PLANE * depth
    chunk = sizes["chunk"]
    me = lax.axis_index("fs")
    core = lax.axis_index("tp")
    z = me // PLANE
    p = me % PLANE
    other = 1 - core
    f32, bf16 = jnp.float32, jnp.bfloat16

    def span(start, size, by=128):
        return pl.ds(pl.multiple_of(start, by), size)

    def peer(k):
        return (p + k) % PLANE

    def on_plane(k):
        return {"fs": z * PLANE + peer(k)}

    pair = {"tp": other}

    def remote(src, dst, send, recv, where):
        return pltpu.make_async_remote_copy(
            src_ref=src, dst_ref=dst, send_sem=send, recv_sem=recv, device_id=where, device_id_type=MESH
        )

    barrier = pltpu.get_barrier_semaphore()
    for k in range(1, PLANE):
        pl.semaphore_signal(barrier, inc=1, device_id=on_plane(k), device_id_type=MESH)
    pl.semaphore_signal(barrier, inc=1, device_id=pair, device_id_type=MESH)

    @pl.when(z > 0)
    def _():
        pl.semaphore_signal(barrier, inc=1, device_id={"fs": me - PLANE}, device_id_type=MESH)

    @pl.when(z < lines - 1)
    def _():
        pl.semaphore_signal(barrier, inc=1, device_id={"fs": me + PLANE}, device_id_type=MESH)

    gate_weights[span(me * depth, depth), pl.ds(0, channels)] = content_ref[...].astype(bf16)
    gate_weights[span(me * depth, depth), pl.ds(channels, channels)] = spatial_ref[...].astype(bf16)
    project_full[:, span(me * depth, depth)] = (project_ref[...] * project_scale_ref[...]).astype(bf16)

    @pl.loop(0, up_own.shape[1] // units)
    def _(j):
        up_own[:, span(j * units, units)] = up_ref[:, span(j * units, units)].astype(bf16)
        down_own[span(j * units, units), :] = (
            down_ref[span(j * units, units), :] * down_scale_ref[...]
        ).astype(bf16)

    up_full[span(me * depth, depth), :] = up_ref[:, span(p * units, units)].astype(bf16)
    down_full[:, span(me * depth, depth)] = (
        down_ref[span(p * units, units), :] * down_scale_ref[...]
    ).astype(bf16)
    token_rows[:, span(core * half, half)] = tokens_ref[...]

    along = (z > 0).astype(jnp.int32) + (z < lines - 1).astype(jnp.int32)
    pl.semaphore_wait(barrier, PLANE + along)

    def gate_refs(owner):
        return (
            gate_weights.at[span(owner * depth, depth), :],
            project_full.at[:, span(owner * depth, depth)],
        )

    def gate_line(block, side, step):
        refs = gate_refs(block * PLANE + p)
        return [
            remote(
                refs[a], refs[a], gate_line_send.at[a, side, block], gate_line_recv.at[a, block],
                {"fs": me + step * PLANE},
            )
            for a in range(2)
        ]

    def gate_plane(block, k):
        refs = gate_refs(block * PLANE + p)
        return [
            remote(refs[a], refs[a], gate_send.at[a, block, k], gate_recv.at[a, block, k], on_plane(k))
            for a in range(2)
        ]

    def ff_line(a, block, side, step):
        ref = up_full.at[span(block * band, band), :] if a == 0 else down_full.at[:, span(block * band, band)]
        return remote(
            ref, ref, line_send.at[a, side, block], line_recv.at[a, block], {"fs": me + step * PLANE}
        )

    def swap(a, k):
        if a == 0:
            src = up_own.at[:, span(peer(k) * units, units)]
            dst = up_full.at[span(me * depth, depth), :]
        else:
            src = down_own.at[span(peer(k) * units, units), :]
            dst = down_full.at[:, span(me * depth, depth)]
        return remote(src, dst, swap_send.at[a, k], swap_recv.at[a, k], on_plane(k))

    def swap_arrival(a, k):
        owner = z * PLANE + (p + PLANE - k) % PLANE
        dst = up_full.at[span(owner * depth, depth), :] if a == 0 else down_full.at[:, span(owner * depth, depth)]
        return remote(dst, dst, swap_send.at[a, k], swap_recv.at[a, k], on_plane(k))

    def both_sides(block, make):
        @pl.when(z < lines - 1)
        def _():
            make(block, 0, 1)

        @pl.when(z > 0)
        def _():
            make(block, 1, -1)

    def start_gate(block, side, step):
        for copy in gate_line(block, side, step):
            copy.start()

    token_copy = remote(
        tokens_ref, token_rows.at[:, span(core * half, half)], pair_send.at[0], pair_recv.at[0], pair
    )
    token_copy.start()
    both_sides(z, start_gate)
    for a in range(2):
        for k in range(1, PLANE):
            swap(a, k).start()
    for k in range(1, PLANE):
        for copy in gate_plane(z, k):
            copy.start()

    token_copy.wait()

    def normalize(source, gain_ref, target, first):
        @pl.loop(0, rows // chunk)
        def _(i):
            values = source[span(i * chunk, chunk, chunk), :].astype(f32)
            scaled = values * lax.rsqrt(jnp.mean(values * values, axis=-1, keepdims=True) + EPSILON)
            target[span(first + i * chunk, chunk, chunk), :] = (scaled * gain_ref[...]).astype(bf16)

    normalize(token_rows, mixer_gain_ref, normed, 0)

    for d in range(1, lines):
        for side, step in ((0, 1), (1, -1)):
            block = z - step * d

            @pl.when((block >= 0) & (block < lines))
            def _(block=block, side=side, step=step):
                for copy in gate_line(block, side, step):
                    copy.wait_recv()

                @pl.when((z + step >= 0) & (z + step < lines))
                def _():
                    start_gate(block, side, step)

                for k in range(1, PLANE):
                    for copy in gate_plane(block, k):
                        copy.start()

    for a in range(2):
        for k in range(1, PLANE):
            swap_arrival(a, k).wait_recv()
        both_sides(z, lambda block, side, step, a=a: ff_line(a, block, side, step).start())

    def relay(d, parts, forward):
        for a in parts:
            for side, step in ((0, 1), (1, -1)):
                block = z - step * d

                @pl.when((block >= 0) & (block < lines))
                def _(a=a, block=block, side=side, step=step):
                    ff_line(a, block, side, step).wait_recv()
                    if forward:

                        @pl.when((z + step >= 0) & (z + step < lines))
                        def _():
                            ff_line(a, block, side, step).start()

    if lines > 2:
        relay(1, (0, 1), True)

    def gate_arrival(block, k):
        refs = gate_refs(block * PLANE + (p + PLANE - k) % PLANE)
        return [
            remote(refs[a], refs[a], gate_send.at[a, block, k], gate_recv.at[a, block, k], on_plane(k))
            for a in range(2)
        ]

    for block in range(lines):
        for k in range(1, PLANE):
            for copy in gate_arrival(block, k):
                copy.wait_recv()

    tile = sizes["tile"]

    @pl.loop(0, channels // tile)
    def _(j):
        at = span(j * tile, tile)
        linear = jnp.dot(normed[...], gate_weights[:, at], preferred_element_type=f32)
        content_buf[:, at] = jax.nn.gelu(linear * content_scale_ref[:, at])
        linear = jnp.dot(
            normed[...], gate_weights[:, span(channels + j * tile, tile)], preferred_element_type=f32
        )
        spatial_buf[:, at] = jax.nn.gelu(linear * spatial_scale_ref[:, at])

    spatial = spatial_buf[...]
    sums[...] = jnp.broadcast_to(jnp.sum(spatial * spatial, axis=1, keepdims=True), sums.shape)
    sum_copy = remote(sums, sums_in, pair_send.at[1], pair_recv.at[1], pair)
    sum_copy.start()
    sum_copy.wait()
    groups, block_size = mixing_ref.shape[0], mixing_ref.shape[1]
    group_width = channels // groups
    causal = lax.broadcasted_iota(jnp.int32, (block_size, block_size), 0) >= lax.broadcasted_iota(
        jnp.int32, (block_size, block_size), 1
    )
    for g in range(groups):
        weights = jnp.where(causal, mixing_ref[g].astype(f32), 0.0).astype(bf16)
        bias = jnp.broadcast_to(bias_ref[pl.ds(g, 1), :], (block_size, block_size)).T[:, :1]
        at = pl.ds(g * group_width, group_width)
        for n in range(rows // block_size):
            these = pl.ds(n * block_size, block_size)
            total = (sums[these, :1] + sums_in[these, :1]) / (2 * channels)
            spatial_norm = (
                spatial_buf[these, at] * lax.rsqrt(total + EPSILON) * spatial_gain_ref[:, at]
            ).astype(bf16)
            mixed = jnp.dot(weights, spatial_norm, preferred_element_type=f32) + bias
            gated[these, at] = (content_buf[these, at] * mixed).astype(bf16)

    @pl.loop(0, width // (2 * tile))
    def _(j):
        at = span(j * 2 * tile, 2 * tile)
        part[:, at] = jnp.dot(gated[...], project_full[:, at], preferred_element_type=f32).astype(bf16)

    part_copy = remote(part.at[:, span(other * half, half)], part_in, pair_send.at[2], pair_recv.at[2], pair)
    part_copy.start()
    part_copy.wait()
    mine = span(core * half, half)

    @pl.loop(0, rows // chunk)
    def _(i):
        these = span(i * chunk, chunk, chunk)
        total = part[these, mine].astype(f32) + part_in[these, :].astype(f32)
        middle[these, mine] = (tokens_ref[these, :].astype(f32) + total).astype(bf16)

    middle_copy = remote(middle.at[:, mine], middle.at[:, mine], pair_send.at[3], pair_recv.at[3], pair)
    middle_copy.start()
    middle_copy.wait()
    normalize(middle, channel_gain_ref, rows_all, p * rows)

    own_rows = rows_all.at[span(p * rows, rows), mine]
    row_copies = [remote(own_rows, own_rows, row_send.at[k], row_recv.at[k], on_plane(k)) for k in range(1, PLANE)]
    for copy in row_copies:
        copy.start()

    for d in range(2, lines - 1):
        relay(d, (0, 1), True)

    forwards = []
    for k in range(1, PLANE):
        theirs = rows_all.at[span((p + PLANE - k) % PLANE * rows, rows), mine]
        remote(theirs, theirs, row_send.at[k], row_recv.at[k], on_plane(k)).wait_recv()
        forwards.append(remote(theirs, theirs, fwd_send.at[k], fwd_recv.at[k], pair))
        forwards[-1].start()
    for copy in forwards:
        copy.wait_recv()

    relay(lines - 1, (0,), False)

    up_tile = sizes["up_tile"]

    @pl.loop(0, PLANE)
    def _(r):
        these = span(r * rows, rows)

        @pl.loop(0, units // up_tile)
        def _(j):
            at = span(j * up_tile, up_tile)
            linear = jnp.dot(rows_all[these, :], up_full[:, at], preferred_element_type=f32)
            linear = linear * up_scale_ref[:, span(p * units + j * up_tile, up_tile)]
            hidden[these, at] = jnp.square(jnp.maximum(linear, 0.0)).astype(bf16)

    per_core = lines // 2

    def result_copy(block, k):
        local = block % per_core
        return remote(
            terms.at[block, span(peer(k) * rows, rows), :],
            results_in.at[k, local],
            result_send.at[local, k],
            result_recv.at[local, k],
            on_plane(k),
        )

    def term_copy(block):
        local = block % per_core
        return remote(terms.at[block], terms_in.at[local], term_send.at[local], term_recv.at[local], pair)

    for i in range(lines):
        block = sizes["order"][0][i]
        for row in range(1, lines):
            block = jnp.where(z == row, sizes["order"][row][i], block)
        if i == lines - 1:
            relay(lines - 1, (1,), False)

        @pl.loop(0, PLANE)
        def _(r, block=block):
            these = span(r * rows, rows)
            terms[block, these, :] = jnp.dot(
                hidden[these, :], down_full[:, span(block * band, band)], preferred_element_type=f32
            ).astype(bf16)

        @pl.when(block // per_core != core)
        def _(block=block):
            term_copy(block).start()

        @pl.when(block // per_core == core)
        def _(block=block):
            term_copy(block).wait_recv()
            local = block % per_core

            @pl.loop(0, PLANE * rows // chunk)
            def _(i):
                these = span(i * chunk, chunk, chunk)
                terms[block, these, :] = (
                    terms[block, these, :].astype(f32) + terms_in[local, these, :].astype(f32)
                ).astype(bf16)

            for k in range(1, PLANE):
                result_copy(block, k).start()

    for i in range(per_core):
        block = core * per_core + i
        for k in range(1, PLANE):
            result_copy(block, k).wait_recv()
        at = pl.ds(i * band, band)

        @pl.loop(0, rows // chunk)
        def _(c, block=block, at=at, i=i):
            these = span(c * chunk, chunk, chunk)
            total = terms[block, span(p * rows + c * chunk, chunk, chunk), :].astype(f32)
            for k in range(1, PLANE):
                total = total + results_in[k, i, these, :].astype(f32)
            out_ref[these, at] = (
                middle[these, span(core * half + i * band, band)].astype(f32) + total
            ).astype(bf16)

    for k in range(1, PLANE):
        for a in range(2):
            swap(a, k).wait_send()
        for block in range(lines):
            for copy in gate_plane(block, k):
                copy.wait_send()
        row_copies[k - 1].wait_send()
        forwards[k - 1].wait_send()
        for i in range(per_core):
            result_copy(core * per_core + i, k).wait_send()
    for i in range(per_core):
        term_copy(other * per_core + i).wait_send()
    for side, step in ((0, 1), (1, -1)):
        for d in range(lines):
            block = z - step * d

            @pl.when((block >= 0) & (block < lines) & (z + step >= 0) & (z + step < lines))
            def _(block=block, side=side, step=step):
                for copy in gate_line(block, side, step):
                    copy.wait_send()
                for a in range(2):
                    ff_line(a, block, side, step).wait_send()


def fused_shards(fs, tokens, mixer_gain, w_content, w_spatial, content_scale, spatial_scale, spatial_gain,
                 block_mixing, block_bias, w_project, project_scale, channel_gain, w_up, up_scale, w_down, down_scale):
    lines = fs // PLANE
    rows, half = tokens.shape
    width = 2 * half
    channels = w_content.shape[1]
    hidden_units = w_up.shape[1]
    units = hidden_units // PLANE
    depth = w_up.shape[0]
    band = PLANE * depth
    per_core = lines // 2
    bf16, f32 = jnp.bfloat16, jnp.float32
    order = [sorted(range(lines), key=lambda b, z=z: (abs(b - z), b)) for z in range(lines)]
    sizes = dict(lines=lines, order=order, chunk=64, tile=256, up_tile=256)
    vmem = pltpu.VMEM
    dma = pltpu.SemaphoreType.DMA
    row = lambda a: a.reshape(1, -1)
    return pl.pallas_call(
        functools.partial(layer_kernel, sizes),
        out_shape=jax.ShapeDtypeStruct((rows, half), bf16),
        in_specs=[pl.BlockSpec(memory_space=vmem)] * 16,
        out_specs=pl.BlockSpec(memory_space=vmem),
        scratch_shapes=[
            vmem((rows, width), bf16),
            vmem((rows, width), bf16),
            vmem((width, 2 * channels), bf16),
            vmem((channels, width), bf16),
            vmem((depth, hidden_units), bf16),
            vmem((hidden_units, depth), bf16),
            vmem((width, units), bf16),
            vmem((units, width), bf16),
            vmem((rows, channels), f32),
            vmem((rows, channels), f32),
            vmem((rows, channels), bf16),
            vmem((rows, 128), f32),
            vmem((rows, 128), f32),
            vmem((rows, width), bf16),
            vmem((rows, half), bf16),
            vmem((rows, width), bf16),
            vmem((PLANE * rows, width), bf16),
            vmem((PLANE * rows, units), bf16),
            vmem((lines, PLANE * rows, band), bf16),
            vmem((per_core, PLANE * rows, band), bf16),
            vmem((PLANE, per_core, rows, band), bf16),
            dma((4,)),
            dma((4,)),
            dma((2, PLANE)),
            dma((2, PLANE)),
            dma((2, 2, lines)),
            dma((2, lines)),
            dma((2, 2, lines)),
            dma((2, lines)),
            dma((2, lines, PLANE)),
            dma((2, lines, PLANE)),
            dma((PLANE,)),
            dma((PLANE,)),
            dma((PLANE,)),
            dma((PLANE,)),
            dma((per_core,)),
            dma((per_core,)),
            dma((per_core, PLANE)),
            dma((per_core, PLANE)),
        ],
        compiler_params=pltpu.CompilerParams(
            collective_id=0, has_side_effects=True, vmem_limit_bytes=VMEM_LIMIT
        ),
    )(tokens, row(mixer_gain), w_content, w_spatial, row(content_scale), row(spatial_scale), row(spatial_gain),
      block_mixing, block_bias, w_project, row(project_scale), row(channel_gain), w_up, row(up_scale), w_down,
      row(down_scale))


VMEM_LIMIT = 67043328


def solution(mesh):
    fs, tp = mesh.shape["fs"], mesh.shape["tp"]
    if tp == 2 and fs % (2 * PLANE) == 0 and fs <= 16:
        body = functools.partial(fused_shards, fs)
    else:
        body = shards
    return jax.shard_map(
        body,
        mesh=mesh,
        in_specs=(
            P("fs", "tp"),
            P(),
            P("fs", "tp"),
            P("fs", "tp"),
            P("tp"),
            P("tp"),
            P("tp"),
            P("tp", None, None),
            P("tp", None),
            P("tp", "fs"),
            P("fs"),
            P(),
            P("fs", "tp"),
            P("tp"),
            P("tp", "fs"),
            P("fs"),
        ),
        out_specs=P("fs", "tp"),
        check_vma=False,
    )
```

```python
import functools

import jax
import jax.numpy as jnp
from jax import lax
from jax.experimental import pallas as pl
from jax.experimental.pallas import tpu as pltpu
from jax.sharding import PartitionSpec as P

EPSILON = 1e-06


def normalize_rows(token_rows, gain_vector):
    values = token_rows.astype(jnp.float32)
    scaled = values * lax.rsqrt(jnp.mean(values * values, axis=-1, keepdims=True) + EPSILON)
    return (scaled * gain_vector).astype(jnp.bfloat16)


def shards(
    tokens,
    mixer_gain,
    w_content,
    w_spatial,
    content_scale,
    spatial_scale,
    spatial_gain,
    block_mixing,
    block_bias,
    w_project,
    project_scale,
    channel_gain,
    w_up,
    up_scale,
    w_down,
    down_scale,
):
    content_weight = w_content.astype(jnp.bfloat16)
    spatial_weight = w_spatial.astype(jnp.bfloat16)
    project_weight = w_project.astype(jnp.bfloat16)
    up_weight = w_up.astype(jnp.bfloat16)
    down_weight = w_down.astype(jnp.bfloat16)
    project_full, down_full = (
        lax.all_gather(project_scale, "fs", axis=0, tiled=True),
        lax.all_gather(down_scale, "fs", axis=0, tiled=True),
    )
    gathered_rows = lax.all_gather(tokens, "tp", axis=1, tiled=True)
    normed = normalize_rows(gathered_rows, mixer_gain)
    row_count = gathered_rows.shape[0]
    content_full, spatial_full, project_cols = (
        lax.all_gather(content_weight, "fs", axis=0, tiled=True),
        lax.all_gather(spatial_weight, "fs", axis=0, tiled=True),
        lax.all_gather(project_weight, "fs", axis=1, tiled=True),
    )
    content_linear = jnp.dot(normed, content_full, preferred_element_type=jnp.float32)
    spatial_linear = jnp.dot(normed, spatial_full, preferred_element_type=jnp.float32)
    content = jax.nn.gelu(content_linear * content_scale)
    spatial = jax.nn.gelu(spatial_linear * spatial_scale)
    square_sums = lax.psum(jnp.sum(spatial * spatial, axis=1), "tp")
    total_width = spatial.shape[1] * lax.axis_size("tp")
    spatial_norm = (
        spatial * lax.rsqrt(square_sums / total_width + EPSILON)[:, None] * spatial_gain
    ).astype(jnp.bfloat16)
    groups_here = block_mixing.shape[0]
    block_size = block_mixing.shape[1]
    group_width = spatial_norm.shape[1] // groups_here
    causal_mask = jnp.tril(jnp.ones((block_size, block_size), dtype=bool))
    mixing_weights = jnp.where(causal_mask[None, :, :], block_mixing, jnp.zeros_like(block_mixing))
    grouped = spatial_norm.reshape(row_count // block_size, block_size, groups_here, group_width)
    mixed_block = (
        jnp.einsum("gts,nsgc->ntgc", mixing_weights, grouped, preferred_element_type=jnp.float32)
        + block_bias.T[None, :, :, None]
    )
    gated = (content * mixed_block.reshape(row_count, spatial_norm.shape[1])).astype(jnp.bfloat16)
    mixer_terms = jnp.dot(gated, project_cols, preferred_element_type=jnp.float32) * project_full
    mixer_sum = lax.psum_scatter(
        mixer_terms.astype(jnp.bfloat16), "tp", scatter_dimension=1, tiled=True
    ).astype(jnp.float32)
    middle = (tokens.astype(jnp.float32) + mixer_sum).astype(jnp.bfloat16)
    middle_rows = lax.all_gather(middle, "tp", axis=1, tiled=True)
    channel_normed = normalize_rows(middle_rows, channel_gain)
    up_full, down_cols = (
        lax.all_gather(up_weight, "fs", axis=0, tiled=True),
        lax.all_gather(down_weight, "fs", axis=1, tiled=True),
    )
    up_linear = jnp.dot(channel_normed, up_full, preferred_element_type=jnp.float32)
    hidden = jnp.square(jax.nn.relu(up_linear * up_scale)).astype(jnp.bfloat16)
    channel_terms = jnp.dot(hidden, down_cols, preferred_element_type=jnp.float32) * down_full
    channel_sum = lax.psum_scatter(
        channel_terms.astype(jnp.bfloat16), "tp", scatter_dimension=1, tiled=True
    ).astype(jnp.float32)
    return (middle.astype(jnp.float32) + channel_sum).astype(jnp.bfloat16)


PLANE = 4
MESH = pl.DeviceIdType.MESH


def layer_kernel(
    sizes,
    tokens_ref,
    mixer_gain_ref,
    content_ref,
    spatial_ref,
    content_scale_ref,
    spatial_scale_ref,
    spatial_gain_ref,
    mixing_ref,
    bias_ref,
    project_ref,
    project_scale_ref,
    channel_gain_ref,
    up_ref,
    up_scale_ref,
    down_ref,
    down_scale_ref,
    out_ref,
    token_rows,
    normed,
    gate_weights,
    project_full,
    up_own,
    down_own,
    up_full,
    down_full,
    content_buf,
    spatial_buf,
    gated,
    sums,
    sums_in,
    part,
    part_in,
    middle,
    rows_all,
    hidden,
    terms,
    terms_in,
    results_in,
    pair_send,
    pair_recv,
    swap_send,
    swap_recv,
    line_send,
    line_recv,
    gate_line_send,
    gate_line_recv,
    gate_send,
    gate_recv,
    row_send,
    row_recv,
    fwd_send,
    fwd_recv,
    term_send,
    term_recv,
    result_send,
    result_recv,
):
    lines = sizes["lines"]
    rows, half = tokens_ref.shape
    width = token_rows.shape[1]
    depth = content_ref.shape[0]
    channels = content_ref.shape[1]
    units = up_full.shape[1]
    band = PLANE * depth
    piece = band // 2
    chunk = sizes["chunk"]
    me = lax.axis_index("fs")
    core = lax.axis_index("tp")
    z = me // PLANE
    p = me % PLANE
    other = 1 - core
    f32, bf16 = jnp.float32, jnp.bfloat16

    def span(start, size, by=128):
        return pl.ds(pl.multiple_of(start, by), size)

    def peer(k):
        return (p + k) % PLANE

    def on_plane(k):
        return {"fs": z * PLANE + peer(k)}

    pair = {"tp": other}

    def remote(src, dst, send, recv, where):
        return pltpu.make_async_remote_copy(
            src_ref=src, dst_ref=dst, send_sem=send, recv_sem=recv, device_id=where, device_id_type=MESH
        )

    barrier = pltpu.get_barrier_semaphore()
    for k in range(1, PLANE):
        pl.semaphore_signal(barrier, inc=1, device_id=on_plane(k), device_id_type=MESH)
    pl.semaphore_signal(barrier, inc=1, device_id=pair, device_id_type=MESH)

    @pl.when(z > 0)
    def _():
        pl.semaphore_signal(barrier, inc=1, device_id={"fs": me - PLANE}, device_id_type=MESH)

    @pl.when(z < lines - 1)
    def _():
        pl.semaphore_signal(barrier, inc=1, device_id={"fs": me + PLANE}, device_id_type=MESH)

    gate_weights[span(me * depth, depth), pl.ds(0, channels)] = content_ref[...].astype(bf16)
    gate_weights[span(me * depth, depth), pl.ds(channels, channels)] = spatial_ref[...].astype(bf16)
    project_full[:, span(me * depth, depth)] = (project_ref[...] * project_scale_ref[...]).astype(bf16)

    token_rows[:, span(core * half, half)] = tokens_ref[...]

    along = (z > 0).astype(jnp.int32) + (z < lines - 1).astype(jnp.int32)
    pl.semaphore_wait(barrier, PLANE + along)

    def gate_refs(owner):
        return (
            gate_weights.at[span(owner * depth, depth), :],
            project_full.at[:, span(owner * depth, depth)],
        )

    def gate_line(block, side, step):
        refs = gate_refs(block * PLANE + p)
        return [
            remote(
                refs[a], refs[a], gate_line_send.at[a, side, block], gate_line_recv.at[a, block],
                {"fs": me + step * PLANE},
            )
            for a in range(2)
        ]

    def gate_plane(block, k):
        refs = gate_refs(block * PLANE + p)
        return [
            remote(refs[a], refs[a], gate_send.at[a, block, k], gate_recv.at[a, block, k], on_plane(k))
            for a in range(2)
        ]

    def ff_line(a, block, side, step):
        if a == 0:
            ref = up_full.at[span(block * band, band), :]
        else:
            ref = down_full.at[:, span(block * band + (a - 1) * piece, piece)]
        return remote(
            ref, ref, line_send.at[a, side, block], line_recv.at[a, block], {"fs": me + step * PLANE}
        )

    def swap(a, k):
        if a == 0:
            src = up_own.at[:, span(peer(k) * units, units)]
            dst = up_full.at[span(me * depth, depth), :]
        else:
            src = down_own.at[span(peer(k) * units, units), :]
            dst = down_full.at[:, span(me * depth, depth)]
        return remote(src, dst, swap_send.at[a, k], swap_recv.at[a, k], on_plane(k))

    def swap_arrival(a, k):
        owner = z * PLANE + (p + PLANE - k) % PLANE
        dst = up_full.at[span(owner * depth, depth), :] if a == 0 else down_full.at[:, span(owner * depth, depth)]
        return remote(dst, dst, swap_send.at[a, k], swap_recv.at[a, k], on_plane(k))

    def both_sides(block, make):
        @pl.when(z < lines - 1)
        def _():
            make(block, 0, 1)

        @pl.when(z > 0)
        def _():
            make(block, 1, -1)

    def start_gate(block, side, step):
        for copy in gate_line(block, side, step):
            copy.start()

    token_copy = remote(
        tokens_ref, token_rows.at[:, span(core * half, half)], pair_send.at[0], pair_recv.at[0], pair
    )
    token_copy.start()
    both_sides(z, start_gate)

    @pl.loop(0, up_own.shape[1] // units)
    def _(j):
        up_own[:, span(j * units, units)] = up_ref[:, span(j * units, units)].astype(bf16)
        down_own[span(j * units, units), :] = (
            down_ref[span(j * units, units), :] * down_scale_ref[...]
        ).astype(bf16)

    up_full[span(me * depth, depth), :] = up_ref[:, span(p * units, units)].astype(bf16)
    down_full[:, span(me * depth, depth)] = (
        down_ref[span(p * units, units), :] * down_scale_ref[...]
    ).astype(bf16)
    for a in range(2):
        for k in range(1, PLANE):
            swap(a, k).start()
    for k in range(1, PLANE):
        for copy in gate_plane(z, k):
            copy.start()

    token_copy.wait()

    def normalize(source, gain_ref, target, first):
        @pl.loop(0, rows // chunk)
        def _(i):
            values = source[span(i * chunk, chunk, chunk), :].astype(f32)
            scaled = values * lax.rsqrt(jnp.mean(values * values, axis=-1, keepdims=True) + EPSILON)
            target[span(first + i * chunk, chunk, chunk), :] = (scaled * gain_ref[...]).astype(bf16)

    normalize(token_rows, mixer_gain_ref, normed, 0)

    for d in range(1, lines):
        for side, step in ((0, 1), (1, -1)):
            block = z - step * d

            @pl.when((block >= 0) & (block < lines))
            def _(block=block, side=side, step=step):
                for copy in gate_line(block, side, step):
                    copy.wait_recv()

                @pl.when((z + step >= 0) & (z + step < lines))
                def _():
                    start_gate(block, side, step)

                for k in range(1, PLANE):
                    for copy in gate_plane(block, k):
                        copy.start()

    for a in range(2):
        for k in range(1, PLANE):
            swap_arrival(a, k).wait_recv()
        for b in (0,) if a == 0 else (1, 2):
            both_sides(z, lambda block, side, step, b=b: ff_line(b, block, side, step).start())

    def relay(d, parts, forward):
        for a in parts:
            for side, step in ((0, 1), (1, -1)):
                block = z - step * d

                @pl.when((block >= 0) & (block < lines))
                def _(a=a, block=block, side=side, step=step):
                    ff_line(a, block, side, step).wait_recv()
                    if forward:

                        @pl.when((z + step >= 0) & (z + step < lines))
                        def _():
                            ff_line(a, block, side, step).start()

    if lines > 2:
        relay(1, (0, 1, 2), True)

    def gate_arrival(block, k):
        refs = gate_refs(block * PLANE + (p + PLANE - k) % PLANE)
        return [
            remote(refs[a], refs[a], gate_send.at[a, block, k], gate_recv.at[a, block, k], on_plane(k))
            for a in range(2)
        ]

    for block in range(lines):
        for k in range(1, PLANE):
            for copy in gate_arrival(block, k):
                copy.wait_recv()

    for d in range(2, lines - 1):
        relay(d, (0,), True)

    tile = sizes["tile"]

    @pl.loop(0, channels // tile)
    def _(j):
        at = span(j * tile, tile)
        linear = jnp.dot(normed[...], gate_weights[:, at], preferred_element_type=f32)
        content_buf[:, at] = jax.nn.gelu(linear * content_scale_ref[:, at])
        linear = jnp.dot(
            normed[...], gate_weights[:, span(channels + j * tile, tile)], preferred_element_type=f32
        )
        spatial_buf[:, at] = jax.nn.gelu(linear * spatial_scale_ref[:, at])

    spatial = spatial_buf[...]
    sums[...] = jnp.broadcast_to(jnp.sum(spatial * spatial, axis=1, keepdims=True), sums.shape)
    sum_copy = remote(sums, sums_in, pair_send.at[1], pair_recv.at[1], pair)
    sum_copy.start()
    sum_copy.wait()
    groups, block_size = mixing_ref.shape[0], mixing_ref.shape[1]
    group_width = channels // groups
    causal = lax.broadcasted_iota(jnp.int32, (block_size, block_size), 0) >= lax.broadcasted_iota(
        jnp.int32, (block_size, block_size), 1
    )
    for g in range(groups):
        weights = jnp.where(causal, mixing_ref[g].astype(f32), 0.0).astype(bf16)
        bias = jnp.broadcast_to(bias_ref[pl.ds(g, 1), :], (block_size, block_size)).T[:, :1]
        at = pl.ds(g * group_width, group_width)
        for n in range(rows // block_size):
            these = pl.ds(n * block_size, block_size)
            total = (sums[these, :1] + sums_in[these, :1]) / (2 * channels)
            spatial_norm = (
                spatial_buf[these, at] * lax.rsqrt(total + EPSILON) * spatial_gain_ref[:, at]
            ).astype(bf16)
            mixed = jnp.dot(weights, spatial_norm, preferred_element_type=f32) + bias
            gated[these, at] = (content_buf[these, at] * mixed).astype(bf16)

    @pl.loop(0, width // (2 * tile))
    def _(j):
        at = span(j * 2 * tile, 2 * tile)
        part[:, at] = jnp.dot(gated[...], project_full[:, at], preferred_element_type=f32).astype(bf16)

    part_copy = remote(part.at[:, span(other * half, half)], part_in, pair_send.at[2], pair_recv.at[2], pair)
    part_copy.start()
    part_copy.wait()
    mine = span(core * half, half)

    @pl.loop(0, rows // chunk)
    def _(i):
        these = span(i * chunk, chunk, chunk)
        total = part[these, mine].astype(f32) + part_in[these, :].astype(f32)
        middle[these, mine] = (tokens_ref[these, :].astype(f32) + total).astype(bf16)

    middle_copy = remote(middle.at[:, mine], middle.at[:, mine], pair_send.at[3], pair_recv.at[3], pair)
    middle_copy.start()
    middle_copy.wait()
    normalize(middle, channel_gain_ref, rows_all, p * rows)

    own_rows = rows_all.at[span(p * rows, rows), mine]
    row_copies = [remote(own_rows, own_rows, row_send.at[k], row_recv.at[k], on_plane(k)) for k in range(1, PLANE)]
    for copy in row_copies:
        copy.start()

    for d in range(2, lines - 1):
        relay(d, (1, 2), True)
    relay(lines - 1, (0,), False)

    up_tile = sizes["up_tile"]

    def raise_rows(owner):
        these = span(owner * rows, rows)

        @pl.loop(0, units // up_tile)
        def _(j):
            at = span(j * up_tile, up_tile)
            linear = jnp.dot(rows_all[these, :], up_full[:, at], preferred_element_type=f32)
            linear = linear * up_scale_ref[:, span(p * units + j * up_tile, up_tile)]
            hidden[these, at] = jnp.square(jnp.maximum(linear, 0.0)).astype(bf16)

    raise_rows(p)
    forwards = []
    for k in range(1, PLANE):
        theirs = rows_all.at[span((p + PLANE - k) % PLANE * rows, rows), mine]
        remote(theirs, theirs, row_send.at[k], row_recv.at[k], on_plane(k)).wait_recv()
        forwards.append(remote(theirs, theirs, fwd_send.at[k], fwd_recv.at[k], pair))
        forwards[-1].start()
        if k > 1:
            forwards[k - 2].wait_recv()
            raise_rows((p + PLANE - k + 1) % PLANE)
    forwards[-1].wait_recv()
    raise_rows((p + 1) % PLANE)

    per_core = lines

    def result_copy(block, k):
        local = block % per_core
        return remote(
            terms.at[block, span(peer(k) * rows, rows), :],
            results_in.at[k, local],
            result_send.at[local, k],
            result_recv.at[local, k],
            on_plane(k),
        )

    def term_copy(block):
        local = block % per_core
        return remote(terms.at[block], terms_in.at[local], term_send.at[local], term_recv.at[local], pair)

    for i in range(2 * lines):
        block = sizes["order"][0][i // 2]
        for row in range(1, lines):
            block = jnp.where(z == row, sizes["order"][row][i // 2], block)
        block = 2 * block + i % 2
        if i >= 2 * lines - 2:
            relay(lines - 1, (1 + i % 2,), False)

        @pl.loop(0, PLANE)
        def _(r, block=block):
            these = span(r * rows, rows)
            terms[block, these, :] = jnp.dot(
                hidden[these, :], down_full[:, span(block * piece, piece)], preferred_element_type=f32
            ).astype(bf16)

        @pl.when(block // per_core != core)
        def _(block=block):
            term_copy(block).start()

        @pl.when(block // per_core == core)
        def _(block=block):
            term_copy(block).wait_recv()
            local = block % per_core

            @pl.loop(0, PLANE * rows // chunk)
            def _(i):
                these = span(i * chunk, chunk, chunk)
                terms[block, these, :] = (
                    terms[block, these, :].astype(f32) + terms_in[local, these, :].astype(f32)
                ).astype(bf16)

            for k in range(1, PLANE):
                result_copy(block, k).start()

    for i in range(per_core):
        block = core * per_core + i
        for k in range(1, PLANE):
            result_copy(block, k).wait_recv()
        at = pl.ds(i * piece, piece)

        @pl.loop(0, rows // chunk)
        def _(c, block=block, at=at, i=i):
            these = span(c * chunk, chunk, chunk)
            total = terms[block, span(p * rows + c * chunk, chunk, chunk), :].astype(f32)
            for k in range(1, PLANE):
                total = total + results_in[k, i, these, :].astype(f32)
            out_ref[these, at] = (
                middle[these, span(core * half + i * piece, piece)].astype(f32) + total
            ).astype(bf16)

    for k in range(1, PLANE):
        for a in range(2):
            swap(a, k).wait_send()
        for block in range(lines):
            for copy in gate_plane(block, k):
                copy.wait_send()
        row_copies[k - 1].wait_send()
        forwards[k - 1].wait_send()
        for i in range(per_core):
            result_copy(core * per_core + i, k).wait_send()
    for i in range(per_core):
        term_copy(other * per_core + i).wait_send()
    for side, step in ((0, 1), (1, -1)):
        for d in range(lines):
            block = z - step * d

            @pl.when((block >= 0) & (block < lines) & (z + step >= 0) & (z + step < lines))
            def _(block=block, side=side, step=step):
                for copy in gate_line(block, side, step):
                    copy.wait_send()
                for a in range(3):
                    ff_line(a, block, side, step).wait_send()


def fused_shards(fs, tokens, mixer_gain, w_content, w_spatial, content_scale, spatial_scale, spatial_gain,
                 block_mixing, block_bias, w_project, project_scale, channel_gain, w_up, up_scale, w_down, down_scale):
    lines = fs // PLANE
    rows, half = tokens.shape
    width = 2 * half
    channels = w_content.shape[1]
    hidden_units = w_up.shape[1]
    units = hidden_units // PLANE
    depth = w_up.shape[0]
    band = PLANE * depth
    per_core = lines
    piece = band // 2
    bf16, f32 = jnp.bfloat16, jnp.float32
    order = [sorted(range(lines), key=lambda b, z=z: (abs(b - z), b)) for z in range(lines)]
    sizes = dict(lines=lines, order=order, chunk=64, tile=256, up_tile=256)
    vmem = pltpu.VMEM
    dma = pltpu.SemaphoreType.DMA
    row = lambda a: a.reshape(1, -1)
    return pl.pallas_call(
        functools.partial(layer_kernel, sizes),
        out_shape=jax.ShapeDtypeStruct((rows, half), bf16),
        in_specs=[pl.BlockSpec(memory_space=vmem)] * 16,
        out_specs=pl.BlockSpec(memory_space=vmem),
        scratch_shapes=[
            vmem((rows, width), bf16),
            vmem((rows, width), bf16),
            vmem((width, 2 * channels), bf16),
            vmem((channels, width), bf16),
            vmem((depth, hidden_units), bf16),
            vmem((hidden_units, depth), bf16),
            vmem((width, units), bf16),
            vmem((units, width), bf16),
            vmem((rows, channels), f32),
            vmem((rows, channels), f32),
            vmem((rows, channels), bf16),
            vmem((rows, 128), f32),
            vmem((rows, 128), f32),
            vmem((rows, width), bf16),
            vmem((rows, half), bf16),
            vmem((rows, width), bf16),
            vmem((PLANE * rows, width), bf16),
            vmem((PLANE * rows, units), bf16),
            vmem((2 * lines, PLANE * rows, piece), bf16),
            vmem((per_core, PLANE * rows, piece), bf16),
            vmem((PLANE, per_core, rows, piece), bf16),
            dma((4,)),
            dma((4,)),
            dma((2, PLANE)),
            dma((2, PLANE)),
            dma((3, 2, lines)),
            dma((3, lines)),
            dma((2, 2, lines)),
            dma((2, lines)),
            dma((2, lines, PLANE)),
            dma((2, lines, PLANE)),
            dma((PLANE,)),
            dma((PLANE,)),
            dma((PLANE,)),
            dma((PLANE,)),
            dma((per_core,)),
            dma((per_core,)),
            dma((per_core, PLANE)),
            dma((per_core, PLANE)),
        ],
        compiler_params=pltpu.CompilerParams(
            collective_id=0, has_side_effects=True, vmem_limit_bytes=VMEM_LIMIT
        ),
    )(tokens, row(mixer_gain), w_content, w_spatial, row(content_scale), row(spatial_scale), row(spatial_gain),
      block_mixing, block_bias, w_project, row(project_scale), row(channel_gain), w_up, row(up_scale), w_down,
      row(down_scale))


VMEM_LIMIT = 67043328


def solution(mesh):
    fs, tp = mesh.shape["fs"], mesh.shape["tp"]
    if tp == 2 and fs % (2 * PLANE) == 0 and fs <= 16:
        body = functools.partial(fused_shards, fs)
    else:
        body = shards
    return jax.shard_map(
        body,
        mesh=mesh,
        in_specs=(
            P("fs", "tp"),
            P(),
            P("fs", "tp"),
            P("fs", "tp"),
            P("tp"),
            P("tp"),
            P("tp"),
            P("tp", None, None),
            P("tp", None),
            P("tp", "fs"),
            P("fs"),
            P(),
            P("fs", "tp"),
            P("tp"),
            P("tp", "fs"),
            P("fs"),
        ),
        out_specs=P("fs", "tp"),
        check_vma=False,
    )
```

```python
import functools

import jax
import jax.numpy as jnp
from jax import lax
from jax.experimental import pallas as pl
from jax.experimental.pallas import tpu as pltpu
from jax.sharding import PartitionSpec as P

EPSILON = 1e-06


def normalize_rows(token_rows, gain_vector):
    values = token_rows.astype(jnp.float32)
    scaled = values * lax.rsqrt(jnp.mean(values * values, axis=-1, keepdims=True) + EPSILON)
    return (scaled * gain_vector).astype(jnp.bfloat16)


def shards(
    tokens,
    mixer_gain,
    w_content,
    w_spatial,
    content_scale,
    spatial_scale,
    spatial_gain,
    block_mixing,
    block_bias,
    w_project,
    project_scale,
    channel_gain,
    w_up,
    up_scale,
    w_down,
    down_scale,
):
    content_weight = w_content.astype(jnp.bfloat16)
    spatial_weight = w_spatial.astype(jnp.bfloat16)
    project_weight = w_project.astype(jnp.bfloat16)
    up_weight = w_up.astype(jnp.bfloat16)
    down_weight = w_down.astype(jnp.bfloat16)
    project_full, down_full = (
        lax.all_gather(project_scale, "fs", axis=0, tiled=True),
        lax.all_gather(down_scale, "fs", axis=0, tiled=True),
    )
    gathered_rows = lax.all_gather(tokens, "tp", axis=1, tiled=True)
    normed = normalize_rows(gathered_rows, mixer_gain)
    row_count = gathered_rows.shape[0]
    content_full, spatial_full, project_cols = (
        lax.all_gather(content_weight, "fs", axis=0, tiled=True),
        lax.all_gather(spatial_weight, "fs", axis=0, tiled=True),
        lax.all_gather(project_weight, "fs", axis=1, tiled=True),
    )
    content_linear = jnp.dot(normed, content_full, preferred_element_type=jnp.float32)
    spatial_linear = jnp.dot(normed, spatial_full, preferred_element_type=jnp.float32)
    content = jax.nn.gelu(content_linear * content_scale)
    spatial = jax.nn.gelu(spatial_linear * spatial_scale)
    square_sums = lax.psum(jnp.sum(spatial * spatial, axis=1), "tp")
    total_width = spatial.shape[1] * lax.axis_size("tp")
    spatial_norm = (
        spatial * lax.rsqrt(square_sums / total_width + EPSILON)[:, None] * spatial_gain
    ).astype(jnp.bfloat16)
    groups_here = block_mixing.shape[0]
    block_size = block_mixing.shape[1]
    group_width = spatial_norm.shape[1] // groups_here
    causal_mask = jnp.tril(jnp.ones((block_size, block_size), dtype=bool))
    mixing_weights = jnp.where(causal_mask[None, :, :], block_mixing, jnp.zeros_like(block_mixing))
    grouped = spatial_norm.reshape(row_count // block_size, block_size, groups_here, group_width)
    mixed_block = (
        jnp.einsum("gts,nsgc->ntgc", mixing_weights, grouped, preferred_element_type=jnp.float32)
        + block_bias.T[None, :, :, None]
    )
    gated = (content * mixed_block.reshape(row_count, spatial_norm.shape[1])).astype(jnp.bfloat16)
    mixer_terms = jnp.dot(gated, project_cols, preferred_element_type=jnp.float32) * project_full
    mixer_sum = lax.psum_scatter(
        mixer_terms.astype(jnp.bfloat16), "tp", scatter_dimension=1, tiled=True
    ).astype(jnp.float32)
    middle = (tokens.astype(jnp.float32) + mixer_sum).astype(jnp.bfloat16)
    middle_rows = lax.all_gather(middle, "tp", axis=1, tiled=True)
    channel_normed = normalize_rows(middle_rows, channel_gain)
    up_full, down_cols = (
        lax.all_gather(up_weight, "fs", axis=0, tiled=True),
        lax.all_gather(down_weight, "fs", axis=1, tiled=True),
    )
    up_linear = jnp.dot(channel_normed, up_full, preferred_element_type=jnp.float32)
    hidden = jnp.square(jax.nn.relu(up_linear * up_scale)).astype(jnp.bfloat16)
    channel_terms = jnp.dot(hidden, down_cols, preferred_element_type=jnp.float32) * down_full
    channel_sum = lax.psum_scatter(
        channel_terms.astype(jnp.bfloat16), "tp", scatter_dimension=1, tiled=True
    ).astype(jnp.float32)
    return (middle.astype(jnp.float32) + channel_sum).astype(jnp.bfloat16)


PLANE = 4
MESH = pl.DeviceIdType.MESH


def layer_kernel(
    sizes,
    tokens_ref,
    mixer_gain_ref,
    content_ref,
    spatial_ref,
    content_scale_ref,
    spatial_scale_ref,
    spatial_gain_ref,
    mixing_ref,
    bias_ref,
    project_ref,
    project_scale_ref,
    channel_gain_ref,
    up_hbm,
    up_scale_ref,
    down_hbm,
    down_scale_ref,
    out_ref,
    up_ref,
    down_ref,
    load_sem,
    token_rows,
    normed,
    gate_weights,
    project_full,
    up_own,
    down_own,
    up_full,
    down_full,
    content_buf,
    spatial_buf,
    gated,
    sums,
    sums_in,
    part,
    part_in,
    middle,
    rows_all,
    hidden,
    terms,
    terms_in,
    results_in,
    pair_send,
    pair_recv,
    swap_send,
    swap_recv,
    line_send,
    line_recv,
    gate_line_send,
    gate_line_recv,
    gate_send,
    gate_recv,
    row_send,
    row_recv,
    fwd_send,
    fwd_recv,
    term_send,
    term_recv,
    result_send,
    result_recv,
):
    lines = sizes["lines"]
    rows, half = tokens_ref.shape
    width = token_rows.shape[1]
    depth = content_ref.shape[0]
    channels = content_ref.shape[1]
    units = up_full.shape[1]
    band = PLANE * depth
    chunk = sizes["chunk"]
    me = lax.axis_index("fs")
    core = lax.axis_index("tp")
    z = me // PLANE
    p = me % PLANE
    other = 1 - core
    f32, bf16 = jnp.float32, jnp.bfloat16

    def span(start, size, by=128):
        return pl.ds(pl.multiple_of(start, by), size)

    def peer(k):
        return (p + k) % PLANE

    def on_plane(k):
        return {"fs": z * PLANE + peer(k)}

    pair = {"tp": other}

    def remote(src, dst, send, recv, where):
        return pltpu.make_async_remote_copy(
            src_ref=src, dst_ref=dst, send_sem=send, recv_sem=recv, device_id=where, device_id_type=MESH
        )

    loads = [
        pltpu.make_async_copy(up_hbm, up_ref, load_sem.at[0]),
        pltpu.make_async_copy(down_hbm, down_ref, load_sem.at[1]),
    ]
    for load in loads:
        load.start()
    barrier = pltpu.get_barrier_semaphore()
    for k in range(1, PLANE):
        pl.semaphore_signal(barrier, inc=1, device_id=on_plane(k), device_id_type=MESH)
    pl.semaphore_signal(barrier, inc=1, device_id=pair, device_id_type=MESH)

    @pl.when(z > 0)
    def _():
        pl.semaphore_signal(barrier, inc=1, device_id={"fs": me - PLANE}, device_id_type=MESH)

    @pl.when(z < lines - 1)
    def _():
        pl.semaphore_signal(barrier, inc=1, device_id={"fs": me + PLANE}, device_id_type=MESH)

    gate_weights[span(me * depth, depth), pl.ds(0, channels)] = content_ref[...].astype(bf16)
    gate_weights[span(me * depth, depth), pl.ds(channels, channels)] = spatial_ref[...].astype(bf16)
    project_full[:, span(me * depth, depth)] = (project_ref[...] * project_scale_ref[...]).astype(bf16)

    token_rows[:, span(core * half, half)] = tokens_ref[...]

    along = (z > 0).astype(jnp.int32) + (z < lines - 1).astype(jnp.int32)
    pl.semaphore_wait(barrier, PLANE + along)

    def gate_refs(owner):
        return (
            gate_weights.at[span(owner * depth, depth), :],
            project_full.at[:, span(owner * depth, depth)],
        )

    def gate_line(block, side, step):
        refs = gate_refs(block * PLANE + p)
        return [
            remote(
                refs[a], refs[a], gate_line_send.at[a, side, block], gate_line_recv.at[a, block],
                {"fs": me + step * PLANE},
            )
            for a in range(2)
        ]

    def gate_plane(block, k):
        refs = gate_refs(block * PLANE + p)
        return [
            remote(refs[a], refs[a], gate_send.at[a, block, k], gate_recv.at[a, block, k], on_plane(k))
            for a in range(2)
        ]

    def ff_line(a, block, side, step):
        ref = up_full.at[span(block * band, band), :] if a == 0 else down_full.at[:, span(block * band, band)]
        return remote(
            ref, ref, line_send.at[a, side, block], line_recv.at[a, block], {"fs": me + step * PLANE}
        )

    def swap(a, k):
        if a == 0:
            src = up_own.at[:, span(peer(k) * units, units)]
            dst = up_full.at[span(me * depth, depth), :]
        else:
            src = down_own.at[span(peer(k) * units, units), :]
            dst = down_full.at[:, span(me * depth, depth)]
        return remote(src, dst, swap_send.at[a, k], swap_recv.at[a, k], on_plane(k))

    def swap_arrival(a, k):
        owner = z * PLANE + (p + PLANE - k) % PLANE
        dst = up_full.at[span(owner * depth, depth), :] if a == 0 else down_full.at[:, span(owner * depth, depth)]
        return remote(dst, dst, swap_send.at[a, k], swap_recv.at[a, k], on_plane(k))

    def both_sides(block, make):
        @pl.when(z < lines - 1)
        def _():
            make(block, 0, 1)

        @pl.when(z > 0)
        def _():
            make(block, 1, -1)

    def start_gate(block, side, step):
        for copy in gate_line(block, side, step):
            copy.start()

    token_copy = remote(
        tokens_ref, token_rows.at[:, span(core * half, half)], pair_send.at[0], pair_recv.at[0], pair
    )
    token_copy.start()
    both_sides(z, start_gate)
    for load in loads:
        load.wait()

    @pl.loop(0, up_own.shape[1] // units)
    def _(j):
        up_own[:, span(j * units, units)] = up_ref[:, span(j * units, units)].astype(bf16)
        down_own[span(j * units, units), :] = (
            down_ref[span(j * units, units), :] * down_scale_ref[...]
        ).astype(bf16)

    up_full[span(me * depth, depth), :] = up_ref[:, span(p * units, units)].astype(bf16)
    down_full[:, span(me * depth, depth)] = (
        down_ref[span(p * units, units), :] * down_scale_ref[...]
    ).astype(bf16)
    for a in range(2):
        for k in range(1, PLANE):
            swap(a, k).start()
    for k in range(1, PLANE):
        for copy in gate_plane(z, k):
            copy.start()

    token_copy.wait()

    def normalize(source, gain_ref, target, first):
        @pl.loop(0, rows // chunk)
        def _(i):
            values = source[span(i * chunk, chunk, chunk), :].astype(f32)
            scaled = values * lax.rsqrt(jnp.mean(values * values, axis=-1, keepdims=True) + EPSILON)
            target[span(first + i * chunk, chunk, chunk), :] = (scaled * gain_ref[...]).astype(bf16)

    normalize(token_rows, mixer_gain_ref, normed, 0)

    for d in range(1, lines):
        for side, step in ((0, 1), (1, -1)):
            block = z - step * d

            @pl.when((block >= 0) & (block < lines))
            def _(block=block, side=side, step=step):
                for copy in gate_line(block, side, step):
                    copy.wait_recv()

                @pl.when((z + step >= 0) & (z + step < lines))
                def _():
                    start_gate(block, side, step)

                for k in range(1, PLANE):
                    for copy in gate_plane(block, k):
                        copy.start()

    for a in range(2):
        for k in range(1, PLANE):
            swap_arrival(a, k).wait_recv()
        both_sides(z, lambda block, side, step, a=a: ff_line(a, block, side, step).start())

    def relay(d, parts, forward):
        for a in parts:
            for side, step in ((0, 1), (1, -1)):
                block = z - step * d

                @pl.when((block >= 0) & (block < lines))
                def _(a=a, block=block, side=side, step=step):
                    ff_line(a, block, side, step).wait_recv()
                    if forward:

                        @pl.when((z + step >= 0) & (z + step < lines))
                        def _():
                            ff_line(a, block, side, step).start()

    if lines > 2:
        relay(1, (0, 1), True)

    def gate_arrival(block, k):
        refs = gate_refs(block * PLANE + (p + PLANE - k) % PLANE)
        return [
            remote(refs[a], refs[a], gate_send.at[a, block, k], gate_recv.at[a, block, k], on_plane(k))
            for a in range(2)
        ]

    for block in range(lines):
        for k in range(1, PLANE):
            for copy in gate_arrival(block, k):
                copy.wait_recv()

    tile = sizes["tile"]

    @pl.loop(0, channels // tile)
    def _(j):
        at = span(j * tile, tile)
        linear = jnp.dot(normed[...], gate_weights[:, at], preferred_element_type=f32)
        content_buf[:, at] = jax.nn.gelu(linear * content_scale_ref[:, at])
        linear = jnp.dot(
            normed[...], gate_weights[:, span(channels + j * tile, tile)], preferred_element_type=f32
        )
        spatial_buf[:, at] = jax.nn.gelu(linear * spatial_scale_ref[:, at])

    spatial = spatial_buf[...]
    sums[...] = jnp.broadcast_to(jnp.sum(spatial * spatial, axis=1, keepdims=True), sums.shape)
    sum_copy = remote(sums, sums_in, pair_send.at[1], pair_recv.at[1], pair)
    sum_copy.start()
    sum_copy.wait()
    groups, block_size = mixing_ref.shape[0], mixing_ref.shape[1]
    group_width = channels // groups
    causal = lax.broadcasted_iota(jnp.int32, (block_size, block_size), 0) >= lax.broadcasted_iota(
        jnp.int32, (block_size, block_size), 1
    )
    for g in range(groups):
        weights = jnp.where(causal, mixing_ref[g].astype(f32), 0.0).astype(bf16)
        bias = jnp.broadcast_to(bias_ref[pl.ds(g, 1), :], (block_size, block_size)).T[:, :1]
        at = pl.ds(g * group_width, group_width)
        for n in range(rows // block_size):
            these = pl.ds(n * block_size, block_size)
            total = (sums[these, :1] + sums_in[these, :1]) / (2 * channels)
            spatial_norm = (
                spatial_buf[these, at] * lax.rsqrt(total + EPSILON) * spatial_gain_ref[:, at]
            ).astype(bf16)
            mixed = jnp.dot(weights, spatial_norm, preferred_element_type=f32) + bias
            gated[these, at] = (content_buf[these, at] * mixed).astype(bf16)

    @pl.loop(0, width // (2 * tile))
    def _(j):
        at = span(j * 2 * tile, 2 * tile)
        part[:, at] = jnp.dot(gated[...], project_full[:, at], preferred_element_type=f32).astype(bf16)

    part_copy = remote(part.at[:, span(other * half, half)], part_in, pair_send.at[2], pair_recv.at[2], pair)
    part_copy.start()
    part_copy.wait()
    mine = span(core * half, half)

    @pl.loop(0, rows // chunk)
    def _(i):
        these = span(i * chunk, chunk, chunk)
        total = part[these, mine].astype(f32) + part_in[these, :].astype(f32)
        middle[these, mine] = (tokens_ref[these, :].astype(f32) + total).astype(bf16)

    middle_copy = remote(middle.at[:, mine], middle.at[:, mine], pair_send.at[3], pair_recv.at[3], pair)
    middle_copy.start()
    middle_copy.wait()
    normalize(middle, channel_gain_ref, rows_all, p * rows)

    own_rows = rows_all.at[span(p * rows, rows), mine]
    row_copies = [remote(own_rows, own_rows, row_send.at[k], row_recv.at[k], on_plane(k)) for k in range(1, PLANE)]
    for copy in row_copies:
        copy.start()

    for d in range(2, lines - 1):
        relay(d, (0, 1), True)

    forwards = []
    for k in range(1, PLANE):
        theirs = rows_all.at[span((p + PLANE - k) % PLANE * rows, rows), mine]
        remote(theirs, theirs, row_send.at[k], row_recv.at[k], on_plane(k)).wait_recv()
        forwards.append(remote(theirs, theirs, fwd_send.at[k], fwd_recv.at[k], pair))
        forwards[-1].start()
    for copy in forwards:
        copy.wait_recv()

    relay(lines - 1, (0,), False)

    up_tile = sizes["up_tile"]

    @pl.loop(0, PLANE)
    def _(r):
        these = span(r * rows, rows)

        @pl.loop(0, units // up_tile)
        def _(j):
            at = span(j * up_tile, up_tile)
            linear = jnp.dot(rows_all[these, :], up_full[:, at], preferred_element_type=f32)
            linear = linear * up_scale_ref[:, span(p * units + j * up_tile, up_tile)]
            hidden[these, at] = jnp.square(jnp.maximum(linear, 0.0)).astype(bf16)

    per_core = lines // 2

    def result_copy(block, k):
        local = block % per_core
        return remote(
            terms.at[block, span(peer(k) * rows, rows), :],
            results_in.at[k, local],
            result_send.at[local, k],
            result_recv.at[local, k],
            on_plane(k),
        )

    def term_copy(block):
        local = block % per_core
        return remote(terms.at[block], terms_in.at[local], term_send.at[local], term_recv.at[local], pair)

    for i in range(lines):
        block = sizes["order"][0][i]
        for row in range(1, lines):
            block = jnp.where(z == row, sizes["order"][row][i], block)
        if i == lines - 1:
            relay(lines - 1, (1,), False)

        @pl.loop(0, PLANE)
        def _(r, block=block):
            these = span(r * rows, rows)
            terms[block, these, :] = jnp.dot(
                hidden[these, :], down_full[:, span(block * band, band)], preferred_element_type=f32
            ).astype(bf16)

        @pl.when(block // per_core != core)
        def _(block=block):
            term_copy(block).start()

        @pl.when(block // per_core == core)
        def _(block=block):
            term_copy(block).wait_recv()
            local = block % per_core

            @pl.loop(0, PLANE * rows // chunk)
            def _(i):
                these = span(i * chunk, chunk, chunk)
                terms[block, these, :] = (
                    terms[block, these, :].astype(f32) + terms_in[local, these, :].astype(f32)
                ).astype(bf16)

            for k in range(1, PLANE):
                result_copy(block, k).start()

    for i in range(per_core):
        block = core * per_core + i
        for k in range(1, PLANE):
            result_copy(block, k).wait_recv()
        at = pl.ds(i * band, band)

        @pl.loop(0, rows // chunk)
        def _(c, block=block, at=at, i=i):
            these = span(c * chunk, chunk, chunk)
            total = terms[block, span(p * rows + c * chunk, chunk, chunk), :].astype(f32)
            for k in range(1, PLANE):
                total = total + results_in[k, i, these, :].astype(f32)
            out_ref[these, at] = (
                middle[these, span(core * half + i * band, band)].astype(f32) + total
            ).astype(bf16)

    for k in range(1, PLANE):
        for a in range(2):
            swap(a, k).wait_send()
        for block in range(lines):
            for copy in gate_plane(block, k):
                copy.wait_send()
        row_copies[k - 1].wait_send()
        forwards[k - 1].wait_send()
        for i in range(per_core):
            result_copy(core * per_core + i, k).wait_send()
    for i in range(per_core):
        term_copy(other * per_core + i).wait_send()
    for side, step in ((0, 1), (1, -1)):
        for d in range(lines):
            block = z - step * d

            @pl.when((block >= 0) & (block < lines) & (z + step >= 0) & (z + step < lines))
            def _(block=block, side=side, step=step):
                for copy in gate_line(block, side, step):
                    copy.wait_send()
                for a in range(2):
                    ff_line(a, block, side, step).wait_send()


def fused_shards(fs, tokens, mixer_gain, w_content, w_spatial, content_scale, spatial_scale, spatial_gain,
                 block_mixing, block_bias, w_project, project_scale, channel_gain, w_up, up_scale, w_down, down_scale):
    lines = fs // PLANE
    rows, half = tokens.shape
    width = 2 * half
    channels = w_content.shape[1]
    hidden_units = w_up.shape[1]
    units = hidden_units // PLANE
    depth = w_up.shape[0]
    band = PLANE * depth
    per_core = lines // 2
    bf16, f32 = jnp.bfloat16, jnp.float32
    order = [sorted(range(lines), key=lambda b, z=z: (abs(b - z), b)) for z in range(lines)]
    sizes = dict(lines=lines, order=order, chunk=64, tile=256, up_tile=256)
    vmem = pltpu.VMEM
    dma = pltpu.SemaphoreType.DMA
    row = lambda a: a.reshape(1, -1)
    return pl.pallas_call(
        functools.partial(layer_kernel, sizes),
        out_shape=jax.ShapeDtypeStruct((rows, half), bf16),
        in_specs=[
            pl.BlockSpec(memory_space=pl.ANY if i in (12, 14) else vmem) for i in range(16)
        ],
        out_specs=pl.BlockSpec(memory_space=vmem),
        scratch_shapes=[
            vmem((depth, hidden_units), f32),
            vmem((hidden_units, depth), f32),
            dma((2,)),
            vmem((rows, width), bf16),
            vmem((rows, width), bf16),
            vmem((width, 2 * channels), bf16),
            vmem((channels, width), bf16),
            vmem((depth, hidden_units), bf16),
            vmem((hidden_units, depth), bf16),
            vmem((width, units), bf16),
            vmem((units, width), bf16),
            vmem((rows, channels), f32),
            vmem((rows, channels), f32),
            vmem((rows, channels), bf16),
            vmem((rows, 128), f32),
            vmem((rows, 128), f32),
            vmem((rows, width), bf16),
            vmem((rows, half), bf16),
            vmem((rows, width), bf16),
            vmem((PLANE * rows, width), bf16),
            vmem((PLANE * rows, units), bf16),
            vmem((lines, PLANE * rows, band), bf16),
            vmem((per_core, PLANE * rows, band), bf16),
            vmem((PLANE, per_core, rows, band), bf16),
            dma((4,)),
            dma((4,)),
            dma((2, PLANE)),
            dma((2, PLANE)),
            dma((2, 2, lines)),
            dma((2, lines)),
            dma((2, 2, lines)),
            dma((2, lines)),
            dma((2, lines, PLANE)),
            dma((2, lines, PLANE)),
            dma((PLANE,)),
            dma((PLANE,)),
            dma((PLANE,)),
            dma((PLANE,)),
            dma((per_core,)),
            dma((per_core,)),
            dma((per_core, PLANE)),
            dma((per_core, PLANE)),
        ],
        compiler_params=pltpu.CompilerParams(
            collective_id=0, has_side_effects=True, vmem_limit_bytes=VMEM_LIMIT
        ),
    )(tokens, row(mixer_gain), w_content, w_spatial, row(content_scale), row(spatial_scale), row(spatial_gain),
      block_mixing, block_bias, w_project, row(project_scale), row(channel_gain), w_up, row(up_scale), w_down,
      row(down_scale))


VMEM_LIMIT = 67043328


def solution(mesh):
    fs, tp = mesh.shape["fs"], mesh.shape["tp"]
    if tp == 2 and fs % (2 * PLANE) == 0 and fs <= 16:
        body = functools.partial(fused_shards, fs)
    else:
        body = shards
    return jax.shard_map(
        body,
        mesh=mesh,
        in_specs=(
            P("fs", "tp"),
            P(),
            P("fs", "tp"),
            P("fs", "tp"),
            P("tp"),
            P("tp"),
            P("tp"),
            P("tp", None, None),
            P("tp", None),
            P("tp", "fs"),
            P("fs"),
            P(),
            P("fs", "tp"),
            P("tp"),
            P("tp", "fs"),
            P("fs"),
        ),
        out_specs=P("fs", "tp"),
        check_vma=False,
    )
```
